32 devices in a mesh: sp: 8 (over z, y), tp: 4 (over x, core).
Axes of the slice: x: 2, y: 2, z: 4, core: 2. Of those that a mesh axis runs over, the one named last changes fastest.
Arguments:
- tokens: bfloat16 [3072, 2048], P('sp', 'tp'), may hold values from -16 to 16
- norm_gain: bfloat16 [2048], replicated, may hold values from 0.099609375 to 1.8984375
- w_query: bfloat16 [2048, 1024], P(None, 'tp'), may hold values from -0.125 to 0.125
- w_key: bfloat16 [2048, 1024], P(None, 'tp'), may hold values from -0.125 to 0.125
- w_value: bfloat16 [2048, 1024], P(None, 'tp'), may hold values from -0.125 to 0.125
- key_bias: bfloat16 [8, 3072], P('tp', 'sp'), may hold values from -13 to 0
- w_glu_value: bfloat16 [2048, 1024], P(None, 'tp'), may hold values from -0.125 to 0.125
- w_glu_gate: bfloat16 [2048, 1024], P(None, 'tp'), may hold values from -0.125 to 0.125
- conv_weight: bfloat16 [31, 1024], replicated, may hold values from -4 to 4
- conv_bias: bfloat16 [1024], replicated, may hold values from 0 to 16
- ln_gain: bfloat16 [1024], replicated, may hold values from 0.099609375 to 1.8984375
- w_out_att: bfloat16 [1024, 2048], replicated, may hold values from -0.75 to 0.75
- w_out_conv: bfloat16 [1024, 2048], replicated, may hold values from -0.1875 to 0.1875
Outputs:
- mixed: bfloat16 [3072, 2048], P(('sp', 'tp'))
- weight_log: float32 [8, 3072], P('tp', 'sp')
The draws below stay inside these ranges and needn't reach their ends.
All inputs are finite; a program needn't handle non-finite values.
Results may differ from the reference program's by a relative error of at most 0.007.
Values may be sent and summed in bfloat16 or wider, within the bound.
A program may use at most 192 MiB of HBM per device.

```python
import math
import jax
import jax.numpy as jnp
from jax import lax

D = 2048
HEAD = 128
SB_HEADS = 8
CF_WIDTH = 1024
KERNEL = 31
TOK_DEV = 384
TOKENS = 3072
SB_WIDTH = 1024


def draw_tokens(key, part):
    base_key, jitter_key = jax.random.split(key, 2)
    columns = jnp.arange(D, dtype=jnp.float32) / D
    jitter = jax.random.uniform(jitter_key, (D,), jnp.float32, -0.25, 0.25)
    column_scale = jnp.exp(math.log(10.0) * (columns - 0.5) + jitter)
    values = jnp.clip(jax.random.normal(base_key, (TOKENS, D), jnp.float32), -6.0, 6.0)
    return jnp.clip(values * column_scale, -16.0, 16.0).astype(jnp.bfloat16)


def draw_key_bias(key, part):
    kind_key, slow_key, quick_random_key, block_key, spot_key, loss_key = jax.random.split(key, 6)
    slow_share = 0.5
    slow_heads = jax.random.uniform(kind_key, (SB_HEADS, 1), jnp.float32) < slow_share
    slow_level = -math.log(TOKENS) - 1.0 + jax.random.uniform(slow_key, (SB_HEADS, 1), jnp.float32, -0.3, 0.3)
    fast_level = jax.random.uniform(quick_random_key, (SB_HEADS, 1), jnp.float32, -4.5, -3.5)
    noise_magnitude = jnp.where(slow_heads, slow_level, fast_level)
    block_shift = jax.random.uniform(block_key, (SB_HEADS, TOKENS // TOK_DEV), jnp.float32, -0.7, 0.7)
    noise_magnitude = noise_magnitude + jnp.repeat(block_shift, TOK_DEV, axis=1)
    chosen_locations = jax.random.randint(spot_key, (SB_HEADS, 3, 1), 0, TOKENS)
    token_positions = jnp.arange(TOKENS, dtype=jnp.int32)
    sudden_spike = jnp.any(token_positions[None, None, :] == chosen_locations, axis=1)
    loss_terms = jax.random.uniform(loss_key, (SB_HEADS, TOKENS), jnp.float32, -2.0, -0.8)
    return jnp.where(sudden_spike, loss_terms, noise_magnitude).astype(jnp.bfloat16)


def draw_conv_weight(key, part):
    base_key, jitter_key = jax.random.split(key)
    channels = jnp.arange(CF_WIDTH, dtype=jnp.float32) / CF_WIDTH
    jitter = jax.random.uniform(jitter_key, (CF_WIDTH,), jnp.float32, -0.25, 0.25)
    channel_scale = jnp.exp(math.log(10.0) * (channels - 0.5) + jitter)
    values = jnp.clip(jax.random.normal(base_key, (KERNEL, CF_WIDTH), jnp.float32), -6.0, 6.0)
    return jnp.clip(values * channel_scale / math.sqrt(KERNEL), -4.0, 4.0).astype(jnp.bfloat16)


def draw_conv_bias(key, part):
    factor_key = jax.random.fold_in(key, 17)
    channels = jnp.arange(CF_WIDTH, dtype=jnp.float32) / CF_WIDTH
    factors = jax.random.uniform(factor_key, (CF_WIDTH,), jnp.float32, 0.5, 1.5)
    rising = jnp.exp(math.log(10.0) * channels) * 0.3
    return jnp.clip(rising * factors, 0.0, 16.0).astype(jnp.bfloat16)


def steps_of(own_key, extent, pieces, smallest, high):
    def one(axis_at, shards_of):
        steps = jax.random.uniform(jax.random.fold_in(jax.random.fold_in(own_key, 6), axis_at), (shards_of,), jnp.float32, smallest / len(pieces), high / len(pieces))
        return jnp.repeat(jnp.exp(steps), extent[axis_at] // shards_of).reshape((-1,) + (1,) * (len(extent) - axis_at - 1))

    loudness = one(*pieces[0])
    for cut in pieces[1:]:
        loudness = loudness * one(*cut)
    return loudness


def bell_draw(own_key, dims, deviation, most, cuts=(), kind=jnp.bfloat16):
    entries = jax.random.normal(own_key, dims, jnp.float32) * deviation
    if len(cuts) > 0:
        entries = steps_of(own_key, dims, cuts, -0.22, 0.18) * entries
    return jnp.clip(entries, min=-most, max=most).astype(kind)


def setup_inputs(seed: int = 0) -> dict:
    key_of = jax.random.split(jax.random.key(seed), 14)
    tokens = draw_tokens(jax.random.fold_in(key_of[13], 71), 0)
    norm_gain = jnp.clip(1.0 + 0.18 * jax.random.normal(key_of[1], (D,), jnp.float32), 0.099609375, 1.8984375).astype(jnp.bfloat16)
    w_query = bell_draw(key_of[2], (D, SB_WIDTH), D ** -0.5, 0.125, ((1, 4),))
    w_key = bell_draw(key_of[3], (D, SB_WIDTH), D ** -0.5, 0.125, ((1, 4),))
    w_value = bell_draw(key_of[4], (D, SB_WIDTH), D ** -0.5, 0.125, ((1, 4),))
    key_bias = draw_key_bias(jax.random.fold_in(key_of[13], 71), 0)
    w_glu_value = bell_draw(key_of[6], (D, CF_WIDTH), D ** -0.5, 0.125, ((1, 4),))
    w_glu_gate = bell_draw(key_of[7], (D, CF_WIDTH), D ** -0.5, 0.125, ((1, 4),))
    conv_weight = draw_conv_weight(jax.random.fold_in(key_of[13], 71), 0)
    conv_bias = draw_conv_bias(jax.random.fold_in(key_of[13], 71), 0)
    ln_gain = jnp.clip(1.0 + 0.18 * jax.random.normal(key_of[10], (CF_WIDTH,), jnp.float32), 0.099609375, 1.8984375).astype(jnp.bfloat16)
    w_out_att = bell_draw(key_of[11], (SB_WIDTH, D), (SB_WIDTH // 16) ** -0.5, 0.75)
    w_out_conv = bell_draw(key_of[12], (CF_WIDTH, D), CF_WIDTH ** -0.5, 0.1875)
    return {"tokens": tokens, "norm_gain": norm_gain, "w_query": w_query, "w_key": w_key, "w_value": w_value, "key_bias": key_bias, "w_glu_value": w_glu_value, "w_glu_gate": w_glu_gate, "conv_weight": conv_weight, "conv_bias": conv_bias, "ln_gain": ln_gain, "w_out_att": w_out_att, "w_out_conv": w_out_conv}


epsilon = 1e-06

def rounded(values):
    return lax.optimization_barrier(values.astype(jnp.bfloat16)).astype(jnp.float32)

def later_matrix(count):
    row_ids = lax.broadcasted_iota(jnp.int32, (count, count), 0)
    col_ids = lax.broadcasted_iota(jnp.int32, (count, count), 1)
    return (row_ids > col_ids).astype(jnp.float32)

def block_terms(query_matrix_rows, key_rows, value_rows, bias_rows, causal):
    head_size = query_matrix_rows.shape[-1]
    scores = jnp.einsum('qhe,khe->hqk', query_matrix_rows.astype(jnp.float32), key_rows.astype(jnp.float32))
    scores = scores * head_size ** (-0.5) + bias_rows.astype(jnp.float32)[:, None, :]
    keep_log = jax.nn.log_sigmoid(-scores)
    if causal:
        row_ids = lax.broadcasted_iota(jnp.int32, scores.shape, 1)
        col_ids = lax.broadcasted_iota(jnp.int32, scores.shape, 2)
        allowed = col_ids <= row_ids
        keep_log = jnp.where(allowed, keep_log, 0.0)
    later_sum = jnp.einsum('hqj,jk->hqk', keep_log, later_matrix(scores.shape[2]), precision=lax.Precision.HIGHEST)
    weights = jnp.exp(jax.nn.log_sigmoid(scores) + later_sum)
    if causal:
        weights = jnp.where(allowed, weights, 0.0)
    weights = rounded(weights)
    block_out = jnp.einsum('hqk,khe->qhe', weights, value_rows.astype(jnp.float32))
    return (block_out, lax.optimization_barrier(jnp.sum(keep_log, axis=2)))

def combine(attended_sum, carried, block_out, block_keep):
    factor = jnp.exp(carried).T[:, :, None]
    return (attended_sum + factor * block_out, carried + block_keep)

def reference(tokens, norm_gain, w_query, w_key, w_value, key_bias, w_glu_value, w_glu_gate, conv_weight, conv_bias, ln_gain, w_out_att, w_out_conv):
    flat = tokens.astype(jnp.float32)
    row_scale = lax.rsqrt(lax.optimization_barrier(jnp.mean(flat * flat, axis=1)) + epsilon)
    normed = (flat * row_scale[:, None] * norm_gain.astype(jnp.float32)).astype(jnp.bfloat16)

    def project(matrix):
        return jnp.dot(normed, matrix, preferred_element_type=jnp.float32)
    query_all = project(w_query).astype(jnp.bfloat16).reshape(TOKENS, SB_HEADS, HEAD)
    key_all = project(w_key).astype(jnp.bfloat16).reshape(TOKENS, SB_HEADS, HEAD)
    value_all = project(w_value).astype(jnp.bfloat16).reshape(TOKENS, SB_HEADS, HEAD)
    glu_value = rounded(project(w_glu_value))
    glu_gate = rounded(project(w_glu_gate))

    def one_block(block):
        begin = block * TOK_DEV
        query_matrix_rows = lax.dynamic_slice_in_dim(query_all, begin, TOK_DEV, 0)
        own_state = block_terms(query_matrix_rows, lax.dynamic_slice_in_dim(key_all, begin, TOK_DEV, 0), lax.dynamic_slice_in_dim(value_all, begin, TOK_DEV, 0), lax.dynamic_slice_in_dim(key_bias, begin, TOK_DEV, 1), True)

        def absorb(turn_index, loop_state):
            earlier = (block - turn_index) * TOK_DEV
            block_out, block_keep = block_terms(query_matrix_rows, lax.dynamic_slice_in_dim(key_all, earlier, TOK_DEV, 0), lax.dynamic_slice_in_dim(value_all, earlier, TOK_DEV, 0), lax.dynamic_slice_in_dim(key_bias, earlier, TOK_DEV, 1), False)
            return combine(loop_state[0], loop_state[1], block_out, block_keep)
        return lax.fori_loop(1, block + 1, absorb, own_state)
    blocks = TOKENS // TOK_DEV
    results = lax.map(one_block, jnp.arange(blocks, dtype=jnp.int32))
    attended = results[0].reshape(TOKENS, SB_WIDTH).astype(jnp.bfloat16)
    carried = jnp.transpose(results[1], (1, 0, 2)).reshape(SB_HEADS, TOKENS)
    weight_log = jnp.log(-jnp.expm1(carried))
    gated = (glu_value * jax.nn.sigmoid(glu_gate)).astype(jnp.bfloat16)
    convolved = lax.conv_general_dilated(gated[None], conv_weight[:, None, :], (1,), [(KERNEL - 1, 0)], dimension_numbers=('NWC', 'WIO', 'NWC'), feature_group_count=CF_WIDTH, preferred_element_type=jnp.float32)[0]
    convolved = convolved + conv_bias.astype(jnp.float32)[None, :]
    channel_mean = lax.optimization_barrier(jnp.mean(convolved, axis=1))
    centered = convolved - channel_mean[:, None]
    channel_var = lax.optimization_barrier(jnp.mean(centered * centered, axis=1))
    conv_out = jax.nn.silu(centered * lax.rsqrt(channel_var + epsilon)[:, None] * ln_gain.astype(jnp.float32)).astype(jnp.bfloat16)
    mixed = jnp.dot(attended, w_out_att, preferred_element_type=jnp.float32) + jnp.dot(conv_out, w_out_conv, preferred_element_type=jnp.float32)
    return (mixed.astype(jnp.bfloat16), weight_log)
```

```python
import functools

import jax
import jax.numpy as jnp
from jax import lax
from jax.experimental import pallas as pl
from jax.experimental.pallas import tpu as pltpu
from jax.sharding import PartitionSpec as P

HEAD = 128

epsilon = 1e-06
MESH = pl.DeviceIdType.MESH
VMEM_LIMIT = 56 * 1024 * 1024


def from_behind(block, axis, distance):
    devices = range(lax.axis_size(axis))
    route = [(i - distance, i) for i in devices if i - distance in devices]
    return lax.ppermute(block, axis, route)


def flip(index, bit):
    return index + bit - 2 * bit * ((index // bit) % 2)


def greet(peers, axis):
    barrier = pltpu.get_barrier_semaphore()
    for peer in peers:
        pl.semaphore_signal(barrier, inc=1, device_id={axis: peer}, device_id_type=MESH)
    pl.semaphore_wait(barrier, len(peers))


def project_kernel(
    n, chunks, tok, gain, wq, wk, wv, wgv, wgg, q, k, v, gated, slots, normed, send, recv
):
    me = lax.axis_index("tp")
    rows, width = tok.shape
    step = rows // chunks
    bits = []
    bit = n // 2
    while bit >= 1:
        bits.append(bit)
        bit //= 2
    greet([flip(me, bit) for bit in bits], "tp")

    routes, held = [], [()]
    for bit in bits:
        routes.append(list(held))
        held = held + [path + (bit,) for path in held]

    def owner_of(path):
        owner = me
        for bit in path:
            owner = flip(owner, bit)
        return owner

    index = {}
    for stage, bit in enumerate(bits):
        for path in routes[stage]:
            index[(stage, path)] = len(index)

    def copy_of(stage, path, chunk):
        part = pl.ds(chunk * step, step)
        owner = owner_of(path)
        source = tok.at[part] if path == () else slots.at[owner, part]
        at = index[(stage, path)]
        return pltpu.make_async_remote_copy(
            src_ref=source,
            dst_ref=slots.at[owner, part],
            send_sem=send.at[at, chunk],
            recv_sem=recv.at[at, chunk],
            device_id={"tp": flip(me, bits[stage])},
            device_id_type=MESH,
        )

    for chunk in range(chunks):
        for stage in range(len(bits)):
            copy_of(stage, (), chunk).start()

    def forward(chunk):
        for stage in range(len(bits) - 1):
            for path in routes[stage]:
                copy_of(stage, path, chunk).wait_recv()
                new = path + (bits[stage],)
                for later in range(stage + 1, len(bits)):
                    copy_of(later, new, chunk).start()

    def work(chunk):
        last = len(bits) - 1
        for path in routes[last]:
            copy_of(last, path, chunk).wait_recv()
        part = pl.ds(chunk * step, step)
        squares = jnp.zeros((step, 1), jnp.float32)
        for path in held:
            x = tok[part, :] if path == () else slots[owner_of(path), part, :]
            x = x.astype(jnp.float32)
            squares = squares + jnp.sum(x * x, axis=1, keepdims=True)
        scale = lax.rsqrt(squares / (width * n) + epsilon)
        for path in held:
            owner = owner_of(path)
            x = tok[part, :] if path == () else slots[owner, part, :]
            y = x.astype(jnp.float32) * scale * gain[owner].astype(jnp.float32)
            normed[:, pl.ds(pl.multiple_of(owner * width, width), width)] = y.astype(jnp.bfloat16)

        def project(matrix):
            return jnp.dot(normed[...], matrix[...], preferred_element_type=jnp.float32).astype(
                jnp.bfloat16
            )

        q[part, :] = project(wq)
        k[part, :] = project(wk)
        v[part, :] = project(wv)
        value = project(wgv).astype(jnp.float32)
        gate = project(wgg).astype(jnp.float32)
        gated[part, :] = (value * jax.nn.sigmoid(gate)).astype(jnp.bfloat16)

    for chunk in range(chunks):
        forward(chunk)
        if chunk > 0:
            work(chunk - 1)
    work(chunks - 1)
    for chunk in range(chunks):
        for stage in range(len(bits)):
            for path in routes[stage]:
                copy_of(stage, path, chunk).wait_send()


def attention_tile(q, k, v, bias, later, row_start, masked):
    scores = lax.dot_general(q, k, (((1,), (1,)), ((), ())), preferred_element_type=jnp.float32)
    scores = scores * q.shape[1] ** (-0.5) + bias
    small = jnp.exp(-jnp.abs(scores))
    soft = jnp.where(
        small < 4e-3, small * (1.0 - small * (0.5 - small * (1.0 / 3.0))), jnp.log(1.0 + small)
    )
    keep = jnp.minimum(-scores, 0.0) - soft
    log_weight = jnp.minimum(scores, 0.0) - soft
    if masked:
        row_ids = lax.broadcasted_iota(jnp.int32, scores.shape, 0) + row_start
        col_ids = lax.broadcasted_iota(jnp.int32, scores.shape, 1)
        allowed = col_ids <= row_ids
        keep = jnp.where(allowed, keep, 0.0)
    high = keep.astype(jnp.bfloat16)
    low = (keep - high.astype(jnp.float32)).astype(jnp.bfloat16)
    after = jnp.dot(high, later, preferred_element_type=jnp.float32) + jnp.dot(
        low, later, preferred_element_type=jnp.float32
    )
    weights = jnp.exp(log_weight + after)
    if masked:
        weights = jnp.where(allowed, weights, 0.0)
    out = jnp.dot(weights.astype(jnp.bfloat16), v, preferred_element_type=jnp.float32)
    return out, jnp.sum(keep, axis=1, keepdims=True)


def fill_later(later):
    row_ids = lax.broadcasted_iota(jnp.int32, later.shape, 0)
    col_ids = lax.broadcasted_iota(jnp.int32, later.shape, 1)
    later[...] = (row_ids > col_ids).astype(jnp.float32).astype(jnp.bfloat16)


def attention_kernel(tile, q, k, v, bias, att, carried_out, later, total, carried):
    me = lax.axis_index("sp")
    rows, width = q.shape
    heads = width // HEAD
    fill_later(later)

    def block_step(block, masked):
        begin = pl.multiple_of(block * rows, rows)
        for head in range(heads):
            cols = pl.ds(head * HEAD, HEAD)
            keys = k[pl.ds(begin, rows), cols]
            values = v[pl.ds(begin, rows), cols]
            offsets = bias[block, pl.ds(head, 1), :].astype(jnp.float32)
            for start in range(0, rows, tile):
                part = pl.ds(start, tile)
                out, kept = attention_tile(
                    q[part, cols], keys, values, offsets, later[...], start, masked
                )
                if masked:
                    total[part, cols] = out
                    carried[head, part, :] = kept
                else:
                    before = carried[head, part, :]
                    total[part, cols] = total[part, cols] + jnp.exp(before) * out
                    carried[head, part, :] = before + kept

    block_step(me, True)

    def absorb(turn, state):
        block_step(me - 1 - turn, False)
        return state

    lax.fori_loop(0, me, absorb, 0)
    att[...] = total[...].astype(jnp.bfloat16)
    lanes = lax.broadcasted_iota(jnp.int32, carried_out.shape, 1)
    result = jnp.zeros(carried_out.shape, jnp.float32)
    for head in range(heads):
        result = jnp.where(lanes == head, carried[head], result)
    carried_out[...] = result


def mix_kernel(n, tile, att, conv, gain, wa, wc, out, att_slots, conv_slots, both, send, recv):
    me = lax.axis_index("tp")
    rows, width = att.shape
    channels = conv.shape[1]
    mine = rows // n
    peers = [lax.rem(me + off, n) for off in range(1, n)]
    greet(peers, "tp")

    def copy_of(off, i):
        peer = lax.rem(me + off, n)
        part = pl.ds(pl.multiple_of(peer * mine, mine), mine)
        source, slots = ((conv, conv_slots), (att, att_slots))[i]
        return pltpu.make_async_remote_copy(
            src_ref=source.at[part],
            dst_ref=slots.at[off - 1],
            send_sem=send.at[i, off - 1],
            recv_sem=recv.at[i, off - 1],
            device_id={"tp": peer},
            device_id_type=MESH,
        )

    for i in range(2):
        for off in range(1, n):
            copy_of(off, i).start()
    own = pl.ds(pl.multiple_of(me * mine, mine), mine)
    for off in range(1, n):
        copy_of(off, 0).wait_recv()
    owners = [me] + [lax.rem(me + n - off, n) for off in range(1, n)]
    pieces = [conv[own, :]] + [conv_slots[off - 1] for off in range(1, n)]
    count = n * channels
    mean = sum(jnp.sum(x, axis=1, keepdims=True) for x in pieces) / count
    centered = [x - mean for x in pieces]
    variance = sum(jnp.sum(x * x, axis=1, keepdims=True) for x in centered) / count
    scale = lax.rsqrt(variance + epsilon)
    for owner, x in zip(owners, centered):
        y = x * scale * gain[owner].astype(jnp.float32)
        y = y * jax.nn.sigmoid(y)
        at = pl.multiple_of(n * width + owner * channels, 128)
        both[:, pl.ds(at, channels)] = y.astype(jnp.bfloat16)
    for off in range(1, n):
        copy_of(off, 1).wait_recv()
    for off, owner in enumerate(owners):
        x = att[own, :] if off == 0 else att_slots[off - 1]
        both[:, pl.ds(pl.multiple_of(owner * width, 128), width)] = x
    for start in range(0, out.shape[1], tile):
        cols = pl.ds(start, tile)
        first = jnp.dot(both[:, : n * width], wa[:, cols], preferred_element_type=jnp.float32)
        second = jnp.dot(both[:, n * width :], wc[:, cols], preferred_element_type=jnp.float32)
        out[:, cols] = (first + second).astype(jnp.bfloat16)
    for off in range(1, n):
        for i in range(2):
            copy_of(off, i).wait_send()


def vmem_specs(count):
    return [pl.BlockSpec(memory_space=pltpu.VMEM)] * count


def largest_tile(rows, limit):
    tile = min(rows, limit)
    while rows % tile:
        tile //= 2
    return tile


def on_device(
    tokens,
    norm_gain,
    w_query,
    w_key,
    w_value,
    key_bias,
    w_glu_value,
    w_glu_gate,
    conv_weight,
    conv_bias,
    ln_gain,
    w_out_att,
    w_out_conv,
):
    tok_rows, feature_width = tokens.shape
    n = lax.axis_size("tp")
    sp_count = lax.axis_size("sp")
    tp_index = lax.axis_index("tp")
    width = w_query.shape[1]
    heads_here = width // HEAD
    channels_here = w_glu_value.shape[1]
    model_width = w_out_att.shape[1]
    bf16, f32 = jnp.bfloat16, jnp.float32
    chunks = tok_rows // largest_tile(tok_rows, 128)
    query, key_rows, value_rows, gated = pl.pallas_call(
        functools.partial(project_kernel, n, chunks),
        out_shape=[jax.ShapeDtypeStruct((tok_rows, width), bf16)] * 3
        + [jax.ShapeDtypeStruct((tok_rows, channels_here), bf16)],
        in_specs=vmem_specs(7),
        out_specs=vmem_specs(4),
        scratch_shapes=[
            pltpu.VMEM((n, tok_rows, feature_width), bf16),
            pltpu.VMEM((tok_rows // chunks, n * feature_width), bf16),
            pltpu.SemaphoreType.DMA((n - 1, chunks)),
            pltpu.SemaphoreType.DMA((n - 1, chunks)),
        ],
        compiler_params=pltpu.CompilerParams(
            collective_id=0, has_side_effects=True, vmem_limit_bytes=VMEM_LIMIT
        ),
        name="project",
    )(
        tokens,
        norm_gain.reshape(n, 1, feature_width),
        w_query,
        w_key,
        w_value,
        w_glu_value,
        w_glu_gate,
    )
    rim_width = conv_weight.shape[0] - 1
    rim_rows = from_behind(gated[tok_rows - rim_width :], "sp", 1)
    every_key = lax.all_gather(key_rows, "sp", axis=0, tiled=True)
    every_value = lax.all_gather(value_rows, "sp", axis=0, tiled=True)
    every_bias = lax.all_gather(key_bias, "sp", axis=0, tiled=False)
    channel_start = tp_index * channels_here
    taps_here = lax.dynamic_slice_in_dim(conv_weight, channel_start, channels_here, 1)
    bias_here = lax.dynamic_slice_in_dim(conv_bias, channel_start, channels_here, 0).astype(f32)
    extended = jnp.concatenate([rim_rows, gated], axis=0)
    convolved = lax.conv_general_dilated(
        extended[None],
        taps_here[:, None, :],
        (1,),
        [(0, 0)],
        dimension_numbers=("NWC", "WIO", "NWC"),
        feature_group_count=channels_here,
        preferred_element_type=f32,
    )[0]
    convolved = convolved + bias_here[None, :]
    tile = largest_tile(tok_rows, 128)
    attended, carried = pl.pallas_call(
        functools.partial(attention_kernel, tile),
        out_shape=[
            jax.ShapeDtypeStruct((tok_rows, width), bf16),
            jax.ShapeDtypeStruct((tok_rows, 128), f32),
        ],
        in_specs=vmem_specs(4),
        out_specs=vmem_specs(2),
        scratch_shapes=[
            pltpu.VMEM((tok_rows, tok_rows), bf16),
            pltpu.VMEM((tok_rows, width), f32),
            pltpu.VMEM((heads_here, tok_rows, 1), f32),
        ],
        compiler_params=pltpu.CompilerParams(vmem_limit_bytes=VMEM_LIMIT),
        name="attention",
    )(query, every_key, every_value, every_bias)
    weight_log = jnp.log(-jnp.expm1(carried[:, :heads_here].T))
    mine = tok_rows // n
    mixed = pl.pallas_call(
        functools.partial(mix_kernel, n, largest_tile(model_width, 512)),
        out_shape=jax.ShapeDtypeStruct((mine, model_width), bf16),
        in_specs=vmem_specs(5),
        out_specs=pl.BlockSpec(memory_space=pltpu.VMEM),
        scratch_shapes=[
            pltpu.VMEM((n - 1, mine, width), bf16),
            pltpu.VMEM((n - 1, mine, channels_here), f32),
            pltpu.VMEM((mine, n * (width + channels_here)), bf16),
            pltpu.SemaphoreType.DMA((2, n - 1)),
            pltpu.SemaphoreType.DMA((2, n - 1)),
        ],
        compiler_params=pltpu.CompilerParams(
            collective_id=1, has_side_effects=True, vmem_limit_bytes=VMEM_LIMIT
        ),
        name="mix",
    )(attended, convolved, ln_gain.reshape(n, 1, channels_here), w_out_att, w_out_conv)
    return (mixed, weight_log)


def solution(mesh):
    in_specs = (
        P("sp", "tp"),
        P(),
        P(None, "tp"),
        P(None, "tp"),
        P(None, "tp"),
        P("tp", "sp"),
        P(None, "tp"),
        P(None, "tp"),
        P(),
        P(),
        P(),
        P(),
        P(),
    )
    out_specs = (P(("sp", "tp"), None), P("tp", "sp"))
    return jax.shard_map(
        on_device, mesh=mesh, in_specs=in_specs, out_specs=out_specs, check_vma=False
    )
```

```python
import functools

import jax
import jax.numpy as jnp
from jax import lax
from jax.experimental import pallas as pl
from jax.experimental.pallas import tpu as pltpu
from jax.sharding import PartitionSpec as P

HEAD = 128

epsilon = 1e-06
MESH = pl.DeviceIdType.MESH
VMEM_LIMIT = 56 * 1024 * 1024


def from_behind(block, axis, distance):
    devices = range(lax.axis_size(axis))
    route = [(i - distance, i) for i in devices if i - distance in devices]
    return lax.ppermute(block, axis, route)


def flip(index, bit):
    return index + bit - 2 * bit * ((index // bit) % 2)


def greet(peers, axis):
    barrier = pltpu.get_barrier_semaphore()
    for peer in peers:
        pl.semaphore_signal(barrier, inc=1, device_id={axis: peer}, device_id_type=MESH)
    pl.semaphore_wait(barrier, len(peers))


def project_kernel(
    n, chunks, tok, gain, wq, wk, wv, wgv, wgg, q, k, v, gated, slots, normed, send, recv
):
    me = lax.axis_index("tp")
    rows, width = tok.shape
    step = rows // chunks
    bits = []
    bit = n // 2
    while bit >= 1:
        bits.append(bit)
        bit //= 2
    greet([flip(me, bit) for bit in bits], "tp")

    routes, held = [], [()]
    for bit in bits:
        routes.append(list(held))
        held = held + [path + (bit,) for path in held]

    def owner_of(path):
        owner = me
        for bit in path:
            owner = flip(owner, bit)
        return owner

    index = {}
    for stage, bit in enumerate(bits):
        for path in routes[stage]:
            index[(stage, path)] = len(index)

    def copy_of(stage, path, chunk):
        part = pl.ds(chunk * step, step)
        owner = owner_of(path)
        source = tok.at[part] if path == () else slots.at[owner, part]
        at = index[(stage, path)]
        return pltpu.make_async_remote_copy(
            src_ref=source,
            dst_ref=slots.at[owner, part],
            send_sem=send.at[at, chunk],
            recv_sem=recv.at[at, chunk],
            device_id={"tp": flip(me, bits[stage])},
            device_id_type=MESH,
        )

    for chunk in range(chunks):
        for stage in range(len(bits)):
            copy_of(stage, (), chunk).start()

    def forward(chunk):
        for stage in range(len(bits) - 1):
            for path in routes[stage]:
                copy_of(stage, path, chunk).wait_recv()
                new = path + (bits[stage],)
                for later in range(stage + 1, len(bits)):
                    copy_of(later, new, chunk).start()

    def work(chunk):
        last = len(bits) - 1
        for path in routes[last]:
            copy_of(last, path, chunk).wait_recv()
        part = pl.ds(chunk * step, step)
        squares = jnp.zeros((step, 1), jnp.float32)
        for path in held:
            x = tok[part, :] if path == () else slots[owner_of(path), part, :]
            x = x.astype(jnp.float32)
            squares = squares + jnp.sum(x * x, axis=1, keepdims=True)
        scale = lax.rsqrt(squares / (width * n) + epsilon)
        for path in held:
            owner = owner_of(path)
            x = tok[part, :] if path == () else slots[owner, part, :]
            y = x.astype(jnp.float32) * scale * gain[owner].astype(jnp.float32)
            normed[:, pl.ds(pl.multiple_of(owner * width, width), width)] = y.astype(jnp.bfloat16)

        def project(matrix):
            return jnp.dot(normed[...], matrix[...], preferred_element_type=jnp.float32).astype(
                jnp.bfloat16
            )

        q[part, :] = project(wq)
        k[part, :] = project(wk)
        v[part, :] = project(wv)
        value = project(wgv).astype(jnp.float32)
        gate = project(wgg).astype(jnp.float32)
        gated[part, :] = (value * jax.nn.sigmoid(gate)).astype(jnp.bfloat16)

    for chunk in range(chunks):
        forward(chunk)
        if chunk > 0:
            work(chunk - 1)
    work(chunks - 1)
    for chunk in range(chunks):
        for stage in range(len(bits)):
            for path in routes[stage]:
                copy_of(stage, path, chunk).wait_send()


def attention_tile(q, k, v, bias, later, row_start, masked):
    scores = lax.dot_general(q, k, (((1,), (1,)), ((), ())), preferred_element_type=jnp.float32)
    scores = scores * q.shape[1] ** (-0.5) + bias
    small = jnp.exp(-jnp.abs(scores))
    soft = jnp.where(
        small < 4e-3, small * (1.0 - small * (0.5 - small * (1.0 / 3.0))), jnp.log(1.0 + small)
    )
    keep = jnp.minimum(-scores, 0.0) - soft
    log_weight = jnp.minimum(scores, 0.0) - soft
    if masked:
        row_ids = lax.broadcasted_iota(jnp.int32, scores.shape, 0) + row_start
        col_ids = lax.broadcasted_iota(jnp.int32, scores.shape, 1)
        allowed = col_ids <= row_ids
        keep = jnp.where(allowed, keep, 0.0)
    high = keep.astype(jnp.bfloat16)
    low = (keep - high.astype(jnp.float32)).astype(jnp.bfloat16)
    after = jnp.dot(high, later, preferred_element_type=jnp.float32) + jnp.dot(
        low, later, preferred_element_type=jnp.float32
    )
    weights = jnp.exp(log_weight + after)
    if masked:
        weights = jnp.where(allowed, weights, 0.0)
    out = jnp.dot(weights.astype(jnp.bfloat16), v, preferred_element_type=jnp.float32)
    return out, jnp.sum(keep, axis=1, keepdims=True)


def fill_later(later):
    row_ids = lax.broadcasted_iota(jnp.int32, later.shape, 0)
    col_ids = lax.broadcasted_iota(jnp.int32, later.shape, 1)
    later[...] = (row_ids > col_ids).astype(jnp.float32).astype(jnp.bfloat16)


def place_of(index, n):
    odd = index % 2
    return (1 - odd) * (index // 2) + odd * (n - 1 - index // 2)


def index_at(place, n):
    back = place // (n // 2)
    return (1 - back) * (2 * place) + back * (2 * (n - 1 - place) + 1)


def attention_kernel(
    n, tile, q, k, v, bias, att, carried_out, k_slots, v_slots, b_slots, later, outs, kept,
    carried, send, recv
):
    me = lax.axis_index("sp")
    place = place_of(me, n)
    rows, width = q.shape
    heads = width // HEAD
    half = n // 2
    own = (k, v, bias)
    slots = (k_slots, v_slots, b_slots)

    def seat(distance):
        return index_at((place + distance + n) % n, n)

    sides = (1, -1)
    greet([seat(1), seat(-1)], "sp")

    def copy_of(side, turn, i, first):
        owner = seat(-sides[side] * turn)
        return pltpu.make_async_remote_copy(
            src_ref=own[i] if first else slots[i].at[owner],
            dst_ref=slots[i].at[owner],
            send_sem=send.at[side, i, turn],
            recv_sem=recv.at[side, i, turn],
            device_id={"sp": seat(sides[side])},
            device_id_type=MESH,
        )

    for side in range(2):
        for i in range(3):
            copy_of(side, 0, i, True).start()
    fill_later(later)

    def process(block, refs, masked):
        for head in range(heads):
            cols = pl.ds(head * HEAD, HEAD)
            keys, values = refs[0][:, cols], refs[1][:, cols]
            offsets = refs[2][pl.ds(head, 1), :].astype(jnp.float32)
            for start in range(0, rows, tile):
                part = pl.ds(start, tile)
                out, total = attention_tile(
                    q[part, cols], keys, values, offsets, later[...], start, masked
                )
                outs[block, part, cols] = out
                kept[block, head, part, :] = total

    def absorb(block):
        @pl.when(block < me)
        def _():
            process(block, [slot.at[block] for slot in slots], False)

    process(me, own, True)

    def arrive(side, turn):
        for i in range(3):
            copy_of(side, turn, i, False).wait_recv()

    def onward(side, turn):
        for i in range(3):
            copy_of(side, turn, i, False).start()

    def step(turn, state):
        arrive(0, turn)
        onward(0, turn + 1)
        arrive(1, turn)

        @pl.when(turn < half - 2)
        def _():
            onward(1, turn + 1)

        def each(side, inner):
            absorb(seat((2 * side - 1) * (turn + 1)))
            return inner

        return lax.fori_loop(0, 2, each, state)

    lax.fori_loop(0, half - 1, step, 0)
    arrive(0, half - 1)
    absorb(seat(-half))
    for head in range(heads):
        carried[head] = kept[me, head]

    def combine(turn, state):
        block = me - 1 - turn
        for head in range(heads):
            cols = pl.ds(head * HEAD, HEAD)
            before = carried[head]
            outs[me, :, cols] = outs[me, :, cols] + jnp.exp(before) * outs[block, :, cols]
            carried[head] = before + kept[block, head]
        return state

    lax.fori_loop(0, me, combine, 0)
    att[...] = outs[me].astype(jnp.bfloat16)
    lanes = lax.broadcasted_iota(jnp.int32, carried_out.shape, 1)
    result = jnp.zeros(carried_out.shape, jnp.float32)
    for head in range(heads):
        result = jnp.where(lanes == head, carried[head], result)
    carried_out[...] = result
    for side in range(2):
        for turn in range(half - side):
            for i in range(3):
                copy_of(side, turn, i, turn == 0).wait_send()


def mix_kernel(n, tile, att, conv, gain, wa, wc, out, att_slots, conv_slots, both, send, recv):
    me = lax.axis_index("tp")
    rows, width = att.shape
    channels = conv.shape[1]
    mine = rows // n
    peers = [lax.rem(me + off, n) for off in range(1, n)]
    greet(peers, "tp")

    def copy_of(off, i):
        peer = lax.rem(me + off, n)
        part = pl.ds(pl.multiple_of(peer * mine, mine), mine)
        source, slots = ((conv, conv_slots), (att, att_slots))[i]
        return pltpu.make_async_remote_copy(
            src_ref=source.at[part],
            dst_ref=slots.at[off - 1],
            send_sem=send.at[i, off - 1],
            recv_sem=recv.at[i, off - 1],
            device_id={"tp": peer},
            device_id_type=MESH,
        )

    for i in range(2):
        for off in range(1, n):
            copy_of(off, i).start()
    own = pl.ds(pl.multiple_of(me * mine, mine), mine)
    for off in range(1, n):
        copy_of(off, 0).wait_recv()
    owners = [me] + [lax.rem(me + n - off, n) for off in range(1, n)]
    pieces = [conv[own, :]] + [conv_slots[off - 1] for off in range(1, n)]
    count = n * channels
    mean = sum(jnp.sum(x, axis=1, keepdims=True) for x in pieces) / count
    centered = [x - mean for x in pieces]
    variance = sum(jnp.sum(x * x, axis=1, keepdims=True) for x in centered) / count
    scale = lax.rsqrt(variance + epsilon)
    for owner, x in zip(owners, centered):
        y = x * scale * gain[owner].astype(jnp.float32)
        y = y * jax.nn.sigmoid(y)
        at = pl.multiple_of(n * width + owner * channels, 128)
        both[:, pl.ds(at, channels)] = y.astype(jnp.bfloat16)
    for off in range(1, n):
        copy_of(off, 1).wait_recv()
    for off, owner in enumerate(owners):
        x = att[own, :] if off == 0 else att_slots[off - 1]
        both[:, pl.ds(pl.multiple_of(owner * width, 128), width)] = x
    for start in range(0, out.shape[1], tile):
        cols = pl.ds(start, tile)
        first = jnp.dot(both[:, : n * width], wa[:, cols], preferred_element_type=jnp.float32)
        second = jnp.dot(both[:, n * width :], wc[:, cols], preferred_element_type=jnp.float32)
        out[:, cols] = (first + second).astype(jnp.bfloat16)
    for off in range(1, n):
        for i in range(2):
            copy_of(off, i).wait_send()


def vmem_specs(count):
    return [pl.BlockSpec(memory_space=pltpu.VMEM)] * count


def largest_tile(rows, limit):
    tile = min(rows, limit)
    while rows % tile:
        tile //= 2
    return tile


def on_device(
    tokens,
    norm_gain,
    w_query,
    w_key,
    w_value,
    key_bias,
    w_glu_value,
    w_glu_gate,
    conv_weight,
    conv_bias,
    ln_gain,
    w_out_att,
    w_out_conv,
):
    tok_rows, feature_width = tokens.shape
    n = lax.axis_size("tp")
    sp_count = lax.axis_size("sp")
    tp_index = lax.axis_index("tp")
    width = w_query.shape[1]
    heads_here = width // HEAD
    channels_here = w_glu_value.shape[1]
    model_width = w_out_att.shape[1]
    bf16, f32 = jnp.bfloat16, jnp.float32
    chunks = tok_rows // largest_tile(tok_rows, 128)
    query, key_rows, value_rows, gated = pl.pallas_call(
        functools.partial(project_kernel, n, chunks),
        out_shape=[jax.ShapeDtypeStruct((tok_rows, width), bf16)] * 3
        + [jax.ShapeDtypeStruct((tok_rows, channels_here), bf16)],
        in_specs=vmem_specs(7),
        out_specs=vmem_specs(4),
        scratch_shapes=[
            pltpu.VMEM((n, tok_rows, feature_width), bf16),
            pltpu.VMEM((tok_rows // chunks, n * feature_width), bf16),
            pltpu.SemaphoreType.DMA((n - 1, chunks)),
            pltpu.SemaphoreType.DMA((n - 1, chunks)),
        ],
        compiler_params=pltpu.CompilerParams(
            collective_id=0, has_side_effects=True, vmem_limit_bytes=VMEM_LIMIT
        ),
        name="project",
    )(
        tokens,
        norm_gain.reshape(n, 1, feature_width),
        w_query,
        w_key,
        w_value,
        w_glu_value,
        w_glu_gate,
    )
    rim_width = conv_weight.shape[0] - 1
    rim_rows = from_behind(gated[tok_rows - rim_width :], "sp", 1)
    channel_start = tp_index * channels_here
    taps_here = lax.dynamic_slice_in_dim(conv_weight, channel_start, channels_here, 1)
    bias_here = lax.dynamic_slice_in_dim(conv_bias, channel_start, channels_here, 0).astype(f32)
    extended = jnp.concatenate([rim_rows, gated], axis=0)
    convolved = lax.conv_general_dilated(
        extended[None],
        taps_here[:, None, :],
        (1,),
        [(0, 0)],
        dimension_numbers=("NWC", "WIO", "NWC"),
        feature_group_count=channels_here,
        preferred_element_type=f32,
    )[0]
    convolved = convolved + bias_here[None, :]
    tile = largest_tile(tok_rows, 128)
    attended, carried = pl.pallas_call(
        functools.partial(attention_kernel, sp_count, tile),
        out_shape=[
            jax.ShapeDtypeStruct((tok_rows, width), bf16),
            jax.ShapeDtypeStruct((tok_rows, 128), f32),
        ],
        in_specs=vmem_specs(4),
        out_specs=vmem_specs(2),
        scratch_shapes=[
            pltpu.VMEM((sp_count, tok_rows, width), bf16),
            pltpu.VMEM((sp_count, tok_rows, width), bf16),
            pltpu.VMEM((sp_count, heads_here, tok_rows), bf16),
            pltpu.VMEM((tok_rows, tok_rows), bf16),
            pltpu.VMEM((sp_count, tok_rows, width), f32),
            pltpu.VMEM((sp_count, heads_here, tok_rows, 1), f32),
            pltpu.VMEM((heads_here, tok_rows, 1), f32),
            pltpu.SemaphoreType.DMA((2, 3, sp_count // 2)),
            pltpu.SemaphoreType.DMA((2, 3, sp_count // 2)),
        ],
        compiler_params=pltpu.CompilerParams(
            collective_id=2, has_side_effects=True, vmem_limit_bytes=VMEM_LIMIT
        ),
        name="attention",
    )(query, key_rows, value_rows, key_bias)
    weight_log = jnp.log(-jnp.expm1(carried[:, :heads_here].T))
    mine = tok_rows // n
    mixed = pl.pallas_call(
        functools.partial(mix_kernel, n, largest_tile(model_width, 512)),
        out_shape=jax.ShapeDtypeStruct((mine, model_width), bf16),
        in_specs=vmem_specs(5),
        out_specs=pl.BlockSpec(memory_space=pltpu.VMEM),
        scratch_shapes=[
            pltpu.VMEM((n - 1, mine, width), bf16),
            pltpu.VMEM((n - 1, mine, channels_here), f32),
            pltpu.VMEM((mine, n * (width + channels_here)), bf16),
            pltpu.SemaphoreType.DMA((2, n - 1)),
            pltpu.SemaphoreType.DMA((2, n - 1)),
        ],
        compiler_params=pltpu.CompilerParams(
            collective_id=1, has_side_effects=True, vmem_limit_bytes=VMEM_LIMIT
        ),
        name="mix",
    )(attended, convolved, ln_gain.reshape(n, 1, channels_here), w_out_att, w_out_conv)
    return (mixed, weight_log)


def solution(mesh):
    in_specs = (
        P("sp", "tp"),
        P(),
        P(None, "tp"),
        P(None, "tp"),
        P(None, "tp"),
        P("tp", "sp"),
        P(None, "tp"),
        P(None, "tp"),
        P(),
        P(),
        P(),
        P(),
        P(),
    )
    out_specs = (P(("sp", "tp"), None), P("tp", "sp"))
    return jax.shard_map(
        on_device, mesh=mesh, in_specs=in_specs, out_specs=out_specs, check_vma=False
    )
```
